32 devices in a mesh: grp: 2 (over y), ra: 4 (over z), cb: 4 (over x, core).
Axes of the slice: x: 2, y: 2, z: 4, core: 2. Of those that a mesh axis runs over, the one named last changes fastest.
Arguments:
- tokens: bfloat16 [512, 4096], P('grp', 'cb'), parts along dimension 0, may hold values from -50 to 50
- norm_gains: float32 [3, 4096], P(None, 'cb'), may hold values from 0.1 to 1.9
- gate_weight: float32 [2, 4096, 11264], P(None, 'cb', 'ra'), may hold values from -0.09375 to 0.09375
- value_weight: float32 [2, 4096, 11264], P(None, 'cb', 'ra'), may hold values from -0.09375 to 0.09375
- gate_scale: float32 [2, 11264], P(None, 'ra'), may hold values from 0.3 to 3
- value_scale: float32 [2, 11264], P(None, 'ra'), may hold values from 0.3 to 3
- conv_gate: float32 [2, 3, 11264], P(None, None, 'ra'), may hold values from -3 to 3
- conv_value: float32 [2, 3, 11264], P(None, None, 'ra'), may hold values from -3 to 3
- down_weight: float32 [2, 11264, 4096], P(None, 'ra', 'cb'), may hold values from -0.07537784 to 0.07537784
- down_scale: float32 [2, 4096], P(None, 'cb'), may hold values from 0.3 to 3
Outputs:
- normed_out: bfloat16 [512, 4096], P('grp', 'cb'), parts along dimension 0
The draws below stay inside these ranges and needn't reach their ends.
There are 2 independent parts, one for each index of `grp`. The reference program is written for one: setup_inputs(seed, part) draws one part's arguments, and reference() takes and returns one part's arrays. A program takes and returns all parts, laid end to end along the dimension named above; an argument that names none is the same for every part. Nothing has to cross between parts.
All inputs are finite; a program needn't handle non-finite values.
Results may differ from the reference program's by a relative error of at most 0.012.
The reference program's roundings to bfloat16 on the way count: a program that leaves them out, or rounds other values in their place, can miss the bound.
Values may be sent and summed in bfloat16 or wider, within the bound.
A program may use at most 192 MiB of HBM per device.

```python
import math
import jax
import jax.numpy as jnp
from jax import lax

D = 4096
FF = 11264
TOK = 256
LAYERS = 2
TAPS = 3


def draw_tokens(key, part):
    key_values = jax.random.fold_in(key, 11)
    key_rows = jax.random.fold_in(key, 12)
    col_position = jnp.arange(D, dtype=jnp.float32) / D
    col_scale = 10.0 ** (col_position - 0.5)
    row_scale = 10.0 ** (jax.random.uniform(key_rows, (TOK, 1), jnp.float32) - 0.5)
    values = jnp.clip(jax.random.normal(key_values, (TOK, D), jnp.float32), -5.0, 5.0)
    return (values * row_scale * col_scale).astype(jnp.bfloat16)


def draw_down_weight(key, part):
    key_base = jax.random.fold_in(key, 21)
    unit = FF ** (-0.5)
    base = jnp.clip(jax.random.normal(key_base, (LAYERS, FF, D), jnp.float32), -6.0, 6.0) * unit
    values = base
    return values.astype(jnp.float32)


def steps_of(rng, dims, shards, least, largest):
    loudness = 1.0
    for axis_at, parts in shards:
        heights = jax.random.uniform(jax.random.fold_in(jax.random.fold_in(rng, 6), axis_at), (parts,), jnp.float32, least / len(shards), largest / len(shards))
        loudness = loudness * jnp.repeat(jnp.exp(heights), dims[axis_at] // parts).reshape((-1,) + (1,) * (len(dims) - 1 - axis_at))
    return loudness


def centred(own_key, dims, scale, bound, shards=(), kind=jnp.bfloat16):
    drawn = jax.random.normal(own_key, dims, jnp.float32) * scale
    if len(shards) > 0:
        drawn = steps_of(own_key, dims, shards, -0.22, 0.18) * drawn
    return jnp.clip(drawn, min=-bound, max=bound).astype(kind)


def setup_inputs(seed: int = 0, part: int = 0) -> dict:
    streams_of = jax.random.split(jax.random.key(seed), 11)
    own_keys = jax.random.split(jax.random.fold_in(streams_of[10], part), 11)
    return {
        "tokens": draw_tokens(jax.random.fold_in(jax.random.fold_in(streams_of[10], part), 71), part),
        "norm_gains": jnp.clip(1.0 + 0.18 * jax.random.normal(streams_of[1], (LAYERS + 1, D), jnp.float32), 0.1, 1.9),
        "gate_weight": centred(streams_of[2], (LAYERS, D, FF), D ** -0.5, 0.09375, ((1, 4), (2, 4)), jnp.float32),
        "value_weight": centred(streams_of[3], (LAYERS, D, FF), D ** -0.5, 0.09375, ((1, 4), (2, 4)), jnp.float32),
        "gate_scale": jnp.clip(jnp.exp(math.log(3.0) - 2.3025851 * jax.random.uniform(streams_of[4], (LAYERS, FF), jnp.float32) ** steps_of(streams_of[4], (LAYERS, FF), ((1, 4),), -0.2, 0.2)), 0.3, 3.0),
        "value_scale": jnp.clip(jnp.exp(math.log(3.0) - 2.3025851 * jax.random.uniform(streams_of[5], (LAYERS, FF), jnp.float32) ** steps_of(streams_of[5], (LAYERS, FF), ((1, 4),), -0.2, 0.2)), 0.3, 3.0),
        "conv_gate": centred(streams_of[6], (LAYERS, TAPS, FF), 0.6, 3.0, ((2, 4),), jnp.float32),
        "conv_value": centred(streams_of[7], (LAYERS, TAPS, FF), 0.6, 3.0, ((2, 4),), jnp.float32),
        "down_weight": draw_down_weight(jax.random.fold_in(streams_of[10], 71), part),
        "down_scale": jnp.clip(jnp.exp(math.log(3.0) - 2.3025851 * jax.random.uniform(streams_of[9], (LAYERS, D), jnp.float32) ** steps_of(streams_of[9], (LAYERS, D), ((1, 4),), -0.2, 0.2)), 0.3, 3.0),
    }


epsilon = 1e-06
residual_weight = 0.5

def rms_scale(values):
    return lax.rsqrt(lax.optimization_barrier(jnp.mean(values * values, axis=1, keepdims=True)) + epsilon)

def causal_taps(projected, tap_weights):
    tap_count = tap_weights.shape[0]
    row_count = projected.shape[0]
    padded = jnp.pad(projected, ((tap_count - 1, 0), (0, 0)))
    result = jnp.zeros_like(projected)
    for tap_idx in range(tap_count):
        result = result + padded[tap_idx:tap_idx + row_count] * tap_weights[tap_idx]
    return result

def reference(tokens, norm_gains, gate_weight, value_weight, gate_scale, value_scale, conv_gate, conv_value, down_weight, down_scale):
    current = tokens
    for layer_idx in range(LAYERS):
        state_wide = current.astype(jnp.float32)
        inverse = rms_scale(state_wide)
        scaled = (state_wide * norm_gains[layer_idx]).astype(jnp.bfloat16)
        gate_pre = inverse * gate_scale[layer_idx] * jnp.dot(scaled, gate_weight[layer_idx].astype(jnp.bfloat16), preferred_element_type=jnp.float32)
        value_pre = inverse * value_scale[layer_idx] * jnp.dot(scaled, value_weight[layer_idx].astype(jnp.bfloat16), preferred_element_type=jnp.float32)
        hidden = (jax.nn.gelu(causal_taps(gate_pre, conv_gate[layer_idx]), approximate=True) * causal_taps(value_pre, conv_value[layer_idx])).astype(jnp.bfloat16)
        down_total = jnp.dot(hidden, down_weight[layer_idx].astype(jnp.bfloat16), preferred_element_type=jnp.float32)
        current = (residual_weight * state_wide + down_scale[layer_idx] * down_total).astype(jnp.bfloat16)
    state_wide = current.astype(jnp.float32)
    return (state_wide * rms_scale(state_wide) * norm_gains[LAYERS]).astype(jnp.bfloat16)
```

```python
import functools

import jax
import jax.numpy as jnp
from jax import lax
from jax.experimental import pallas as pl
from jax.experimental.pallas import tpu as pltpu
from jax.sharding import PartitionSpec as P

epsilon = 1e-06
residual_weight = 0.5


def causal_taps(projected, tap_weights):
    tap_count = tap_weights.shape[0]
    row_count = projected.shape[0]
    padded = jnp.pad(projected, ((tap_count - 1, 0), (0, 0)))
    result = jnp.zeros_like(projected)
    for tap_idx in range(tap_count):
        result = result + padded[tap_idx : tap_idx + row_count] * tap_weights[tap_idx]
    return result


def row_inverse(state_wide, model_width):
    squares = lax.psum(jnp.sum(state_wide * state_wide, axis=1, keepdims=True), "cb")
    return lax.rsqrt(squares / model_width + epsilon)


def on_device(
    tokens,
    norm_gains,
    gate_weight,
    value_weight,
    gate_scale,
    value_scale,
    conv_gate,
    conv_value,
    down_weight,
    down_scale,
):
    model_width = lax.axis_size("cb") * tokens.shape[1]
    layer_count = gate_weight.shape[0]
    current = tokens
    for layer_idx in range(layer_count):
        state_wide = current.astype(jnp.float32)
        inverse = row_inverse(state_wide, model_width)
        scaled = (state_wide * norm_gains[layer_idx]).astype(jnp.bfloat16)
        gate_part = jnp.dot(
            scaled, gate_weight[layer_idx].astype(jnp.bfloat16), preferred_element_type=jnp.float32
        )
        value_part = jnp.dot(
            scaled, value_weight[layer_idx].astype(jnp.bfloat16), preferred_element_type=jnp.float32
        )
        gate_sum, value_sum = (
            lax.psum_scatter(gate_part, "cb", scatter_dimension=1, tiled=True),
            lax.psum_scatter(value_part, "cb", scatter_dimension=1, tiled=True),
        )
        share_cols = gate_sum.shape[1]
        first_col = lax.axis_index("cb") * share_cols
        gate_cols = lax.dynamic_slice_in_dim(gate_scale[layer_idx], first_col, share_cols, 0)
        value_cols = lax.dynamic_slice_in_dim(value_scale[layer_idx], first_col, share_cols, 0)
        gate_taps = lax.dynamic_slice_in_dim(conv_gate[layer_idx], first_col, share_cols, 1)
        value_taps = lax.dynamic_slice_in_dim(conv_value[layer_idx], first_col, share_cols, 1)
        gate_pre = inverse * gate_cols * gate_sum
        value_pre = inverse * value_cols * value_sum
        hidden = (
            jax.nn.gelu(causal_taps(gate_pre, gate_taps), approximate=True)
            * causal_taps(value_pre, value_taps)
        ).astype(jnp.bfloat16)
        hidden = lax.all_gather(hidden, "cb", axis=1, tiled=True)
        partial_value = jnp.dot(
            hidden, down_weight[layer_idx].astype(jnp.bfloat16), preferred_element_type=jnp.float32
        )
        down_total = lax.psum(partial_value, "ra")
        current = (residual_weight * state_wide + down_scale[layer_idx] * down_total).astype(
            jnp.bfloat16
        )
    state_wide = current.astype(jnp.float32)
    inverse = row_inverse(state_wide, model_width)
    return (state_wide * inverse * norm_gains[layer_count]).astype(jnp.bfloat16)


HALVES = 2
CORES = 2
LANES = 128
CHUNK = 256
RING = 12
STAGED = 5
BUBBLES = 4
PAIR_SUM, GATED, PAIR_GATHER, DOWN = 1, 4, 7, 8
Z_SUM, Z_GATHER, Z_SCALE = 4, 7, 8


def fused_kernel(
    ra_count,
    cb_count,
    tokens,
    gains,
    gate_hbm,
    value_hbm,
    gate_scale,
    value_scale,
    conv_gate,
    conv_value,
    down_hbm,
    down_scale,
    out,
    gate_stage,
    value_stage,
    down_stage,
    wide_weight,
    down_weight,
    current,
    scaled,
    inverse,
    padded,
    carry,
    pair_send,
    pair_recv,
    pair_own,
    x_send,
    x_recv,
    hidden,
    acc,
    z_send,
    z_recv,
    z_own,
    sq_send,
    sq_recv,
    gate_sem,
    value_sem,
    down_sem,
    pair_ss,
    pair_rs,
    x_ss,
    x_rs,
    hx_ss,
    hx_rs,
    hp_ss,
    hp_rs,
    z_ss,
    z_rs,
    c_ss,
    c_rs,
    sq_ss,
    sq_rs,
):
    f32, bf16 = jnp.float32, jnp.bfloat16
    layers = gate_hbm.shape[0]
    chunks = gate_hbm.shape[2] // CHUNK
    taps = conv_gate.shape[1]
    rows = tokens.shape[1]
    width = tokens.shape[2]
    model_width = width * cb_count
    x_count = cb_count // CORES
    block = rows // cb_count
    z_block = rows // ra_count
    period = HALVES * chunks + BUBBLES
    last_item = layers * period - BUBBLES
    streamed = layers * chunks

    me_cb = lax.axis_index("cb")
    me_ra = lax.axis_index("ra")
    me_x, me_core = lax.div(me_cb, CORES), lax.rem(me_cb, CORES)
    partner = me_x * CORES + (1 - me_core)

    def others(count, me):
        return [lax.rem(me + step, count) for step in range(1, count)]

    def remote(src, dst, send, recv, axis, index):
        return pltpu.make_async_remote_copy(
            src_ref=src,
            dst_ref=dst,
            send_sem=send,
            recv_sem=recv,
            device_id={axis: index},
            device_id_type=pl.DeviceIdType.MESH,
        )

    def cb_of(x_index):
        return x_index * CORES + me_core

    def wide_copies(n):
        layer, chunk, slot = lax.div(n, chunks), lax.rem(n, chunks), lax.rem(n, STAGED)
        cols = pl.ds(pl.multiple_of(chunk * CHUNK, CHUNK), CHUNK)
        return (
            pltpu.make_async_copy(gate_hbm.at[layer, :, cols], gate_stage.at[slot], gate_sem.at[slot]),
            pltpu.make_async_copy(value_hbm.at[layer, :, cols], value_stage.at[slot], value_sem.at[slot]),
        )

    def down_copy(n):
        layer, chunk, slot = lax.div(n, chunks), lax.rem(n, chunks), lax.rem(n, STAGED)
        cols = pl.ds(pl.multiple_of(chunk * CHUNK, CHUNK), CHUNK)
        return pltpu.make_async_copy(down_hbm.at[layer, cols, :], down_stage.at[slot], down_sem.at[slot])

    for n in range(min(STAGED, streamed)):
        for copy in wide_copies(n):
            copy.start()
        down_copy(n).start()

    barrier = pltpu.get_barrier_semaphore()
    for axis, count, me in (("cb", cb_count, me_cb), ("ra", ra_count, me_ra)):
        for peer in others(count, me):
            pl.semaphore_signal(
                barrier, inc=1, device_id={axis: peer}, device_id_type=pl.DeviceIdType.MESH
            )
    pl.semaphore_wait(barrier, cb_count + ra_count - 2)

    def pair_copy(slot):
        return remote(
            pair_send.at[slot], pair_recv.at[slot], pair_ss.at[slot], pair_rs.at[slot], "cb", partner
        )

    def x_copy(slot, peer, source):
        return remote(
            x_send.at[slot, peer],
            x_recv.at[slot, source],
            x_ss.at[slot, peer],
            x_rs.at[slot, source],
            "cb",
            cb_of(peer),
        )

    def hx_copy(slot, peer, source):
        place = hidden.at[slot, me_core * x_count + source]
        return remote(place, place, hx_ss.at[slot, peer], hx_rs.at[slot, source], "cb", cb_of(peer))

    def hp_copy(slot, core):
        place = hidden.at[slot, pl.ds(core * x_count, x_count)]
        return remote(place, place, hp_ss.at[slot], hp_rs.at[slot], "cb", partner)

    def z_copy(part, peer, source):
        return remote(
            z_send.at[part, peer],
            z_recv.at[part, source],
            z_ss.at[part, peer],
            z_rs.at[part, source],
            "ra",
            peer,
        )

    def c_copy(part, layer, half, peer, source):
        place = current.at[layer, half, source]
        return remote(place, place, c_ss.at[part, peer], c_rs.at[part, source], "ra", peer)

    def sq_copy(event, peer, source):
        return remote(
            sq_send.at[event], sq_recv.at[event, source], sq_ss.at[event, peer], sq_rs.at[event, source], "cb", peer
        )

    def scale_rows(layer, half):
        event = layer * HALVES + half
        wide = current[layer, half].reshape(rows, width).astype(f32)
        scaled[half] = (wide * gains[pl.ds(layer, 1), :]).astype(bf16)
        squares = jnp.sum(wide * wide, axis=1, keepdims=True)
        sq_send[event] = jnp.broadcast_to(squares, (rows, LANES)).T[:8]
        for peer in others(cb_count, me_cb):
            sq_copy(event, peer, me_cb).start()

    def finish_squares(layer, half):
        event = layer * HALVES + half
        total = sq_send[event]
        for peer in others(cb_count, me_cb):
            copy = sq_copy(event, peer, peer)
            copy.wait_send()
            copy.wait_recv()
            total = total + sq_recv[event, peer]
        row = lax.rsqrt(total / model_width + epsilon)
        inverse[half] = jnp.broadcast_to(row[:1], (LANES, rows)).T

    for half in range(HALVES):
        current[0, half] = tokens[half].reshape(ra_count, z_block, width)
        scale_rows(0, half)
    for half in range(HALVES):
        finish_squares(0, half)

    def place_of(item):
        layer, rest = lax.div(item, period), lax.rem(item, period)
        half, chunk = lax.div(rest, chunks), lax.rem(rest, chunks)
        ordinal = layer * (HALVES * chunks) + rest
        return layer, half, chunk, lax.rem(ordinal, RING)

    def project(layer, half, chunk, slot):
        n = layer * chunks + chunk

        @pl.when(half == 0)
        def _():
            stage = lax.rem(n, STAGED)
            for copy in wide_copies(n):
                copy.wait()
            wide_weight[chunk, :, :CHUNK] = gate_stage[stage].astype(bf16)
            wide_weight[chunk, :, CHUNK:] = value_stage[stage].astype(bf16)

            @pl.when(n + STAGED < streamed)
            def _():
                for copy in wide_copies(n + STAGED):
                    copy.start()

        product = jnp.dot(scaled[half], wide_weight[chunk], preferred_element_type=f32)
        inv = inverse[half]
        cols = pl.ds(pl.multiple_of(chunk * CHUNK, CHUNK), CHUNK)
        one = pl.ds(layer, 1)
        scales = jnp.concatenate([gate_scale[one, cols], value_scale[one, cols]], axis=1)
        weights = jnp.concatenate([conv_gate[layer, :, cols], conv_value[layer, :, cols]], axis=1)
        wide_inv = jnp.concatenate([inv] * (2 * CHUNK // LANES), axis=1)
        pre = product * wide_inv * scales
        before = carry[chunk]
        padded[:8] = jnp.where(half == 0, jnp.zeros_like(before), before)
        padded[8:] = pre
        carry[chunk] = pre[rows - 8 :]
        total = jnp.zeros_like(pre)
        for tap in range(taps):
            total = total + padded[pl.ds(8 - (taps - 1) + tap, rows), :] * weights[tap : tap + 1]
        part = rows // CORES
        for core in range(CORES):
            piece = total[core * part : (core + 1) * part]

            @pl.when(me_core == core)
            def _():
                pair_own[slot] = piece.reshape(x_count, block, 2 * CHUNK)

            @pl.when(me_core != core)
            def _():
                pair_send[slot] = piece.astype(bf16).reshape(x_count, block, 2 * CHUNK)

        pair_copy(slot).start()

    def pair_sum(layer, half, chunk, slot):
        pair_copy(slot).wait()
        both = pair_own[slot] + pair_recv[slot].astype(f32)
        pair_own[slot] = both
        x_send[slot] = both.astype(bf16)
        for peer in others(x_count, me_x):
            x_copy(slot, peer, me_x).start()

    def gated(layer, half, chunk, slot):
        total = pair_own[slot, me_x]
        for peer in others(x_count, me_x):
            copy = x_copy(slot, peer, peer)
            copy.wait_send()
            copy.wait_recv()
            total = total + x_recv[slot, peer].astype(f32)
        unit = jax.nn.gelu(total[:, :CHUNK], approximate=True) * total[:, CHUNK:]
        hidden[slot, me_core * x_count + me_x] = unit.astype(bf16)
        for peer in others(x_count, me_x):
            hx_copy(slot, peer, me_x).start()

    def pair_gather(layer, half, chunk, slot):
        for peer in others(x_count, me_x):
            hx_copy(slot, peer, me_x).wait_send()
            hx_copy(slot, peer, peer).wait_recv()
        hp_copy(slot, me_core).start()

    def project_down(layer, half, chunk, slot):
        n = layer * chunks + chunk

        @pl.when(half == 0)
        def _():
            stage = lax.rem(n, STAGED)
            down_copy(n).wait()
            down_weight[chunk] = down_stage[stage].astype(bf16)

            @pl.when(n + STAGED < streamed)
            def _():
                down_copy(n + STAGED).start()

        hp_copy(slot, me_core).wait_send()
        hp_copy(slot, 1 - me_core).wait_recv()
        product = jnp.dot(
            hidden[slot].reshape(rows, CHUNK), down_weight[chunk], preferred_element_type=f32
        ).reshape(ra_count, z_block, width)

        @pl.when(chunk == 0)
        def _():
            acc[...] = product

        @pl.when(chunk > 0)
        def _():
            acc[...] += product

        @pl.when(chunk == chunks - 1)
        def _():
            part = layer * HALVES + half
            z_send[part] = acc[...].astype(bf16)
            z_own[part] = acc[me_ra]
            for peer in others(ra_count, me_ra):
                z_copy(part, peer, me_ra).start()

    def z_sum(layer, half, chunk, slot):
        part = layer * HALVES + half
        total = z_own[part]
        for peer in others(ra_count, me_ra):
            copy = z_copy(part, peer, peer)
            copy.wait_send()
            copy.wait_recv()
            total = total + z_recv[part, peer].astype(f32)
        kept = residual_weight * current[layer, half, me_ra].astype(f32)
        current[layer + 1, half, me_ra] = (kept + down_scale[pl.ds(layer, 1), :] * total).astype(bf16)
        for peer in others(ra_count, me_ra):
            c_copy(part, layer + 1, half, peer, me_ra).start()

    def z_gather(layer, half, chunk, slot):
        part = layer * HALVES + half
        for peer in others(ra_count, me_ra):
            c_copy(part, layer + 1, half, peer, me_ra).wait_send()
            c_copy(part, layer + 1, half, peer, peer).wait_recv()
        scale_rows(layer + 1, half)

    def z_scale(layer, half, chunk, slot):
        finish_squares(layer + 1, half)

        @pl.when(layer == layers - 1)
        def _():
            wide = current[layers, half].reshape(rows, width).astype(f32)
            inv = jnp.concatenate([inverse[half]] * (width // LANES), axis=1)
            out[half] = (wide * inv * gains[pl.ds(layers, 1), :]).astype(bf16)

    stages = (
        (DOWN + Z_SCALE, True, z_scale),
        (DOWN + Z_GATHER, True, z_gather),
        (DOWN + Z_SUM, True, z_sum),
        (PAIR_GATHER, False, pair_gather),
        (GATED, False, gated),
        (PAIR_SUM, False, pair_sum),
        (0, False, project),
        (DOWN, False, project_down),
    )
    assert DOWN + Z_SCALE <= chunks + BUBBLES + 1

    def step(index, _):
        for delay, at_end, stage in stages:
            item = index - delay
            rest = lax.rem(item + period, period)
            valid = (item >= 0) & (item < last_item) & (rest < HALVES * chunks)
            if at_end:
                valid = valid & (lax.rem(rest, chunks) == chunks - 1)

            @pl.when(valid)
            def _(stage=stage, item=item):
                stage(*place_of(item))

        return 0

    lax.fori_loop(0, last_item + DOWN + Z_SCALE, step, 0)


def fits(ra_count, cb_count, tokens, gate_weight, conv_gate):
    rows = tokens.shape[0] // HALVES
    return (
        cb_count % CORES == 0
        and cb_count > CORES
        and ra_count > 1
        and tokens.shape[0] % HALVES == 0
        and rows % LANES == 0
        and (rows // LANES) == 1
        and rows % (16 * cb_count) == 0
        and rows % (16 * ra_count) == 0
        and tokens.shape[1] % LANES == 0
        and gate_weight.shape[2] % CHUNK == 0
        and gate_weight.shape[2] // CHUNK + BUBBLES + 1 >= DOWN + Z_SCALE
        and conv_gate.shape[1] <= 9
    )


def on_device_any(ra_count, cb_count, *args):
    (
        tokens,
        norm_gains,
        gate_weight,
        value_weight,
        gate_scale,
        value_scale,
        conv_gate,
        conv_value,
        down_weight,
        down_scale,
    ) = args
    if not fits(ra_count, cb_count, tokens, gate_weight, conv_gate):
        return on_device(*args)
    f32, bf16 = jnp.float32, jnp.bfloat16
    layers, width, units = gate_weight.shape
    rows = tokens.shape[0] // HALVES
    chunks = units // CHUNK
    x_count = cb_count // CORES
    block, z_block = rows // cb_count, rows // ra_count
    parts, events = layers * HALVES, (layers + 1) * HALVES
    vmem, dma = pltpu.VMEM, pltpu.SemaphoreType.DMA
    in_vmem, in_hbm = pl.BlockSpec(memory_space=pltpu.VMEM), pl.BlockSpec(memory_space=pl.ANY)
    result = pl.pallas_call(
        functools.partial(fused_kernel, ra_count, cb_count),
        out_shape=jax.ShapeDtypeStruct((HALVES, rows, width), bf16),
        in_specs=[in_vmem, in_vmem, in_hbm, in_hbm] + [in_vmem] * 4 + [in_hbm, in_vmem],
        out_specs=in_vmem,
        scratch_shapes=[
            vmem((STAGED, width, CHUNK), f32),
            vmem((STAGED, width, CHUNK), f32),
            vmem((STAGED, CHUNK, width), f32),
            vmem((chunks, width, 2 * CHUNK), bf16),
            vmem((chunks, CHUNK, width), bf16),
            vmem((layers + 1, HALVES, ra_count, z_block, width), bf16),
            vmem((HALVES, rows, width), bf16),
            vmem((HALVES, rows, LANES), f32),
            vmem((rows + 8, 2 * CHUNK), f32),
            vmem((chunks, 8, 2 * CHUNK), f32),
            vmem((RING, x_count, block, 2 * CHUNK), bf16),
            vmem((RING, x_count, block, 2 * CHUNK), bf16),
            vmem((RING, x_count, block, 2 * CHUNK), f32),
            vmem((RING, x_count, block, 2 * CHUNK), bf16),
            vmem((RING, x_count, block, 2 * CHUNK), bf16),
            vmem((RING, cb_count, block, CHUNK), bf16),
            vmem((ra_count, z_block, width), f32),
            vmem((parts, ra_count, z_block, width), bf16),
            vmem((parts, ra_count, z_block, width), bf16),
            vmem((parts, z_block, width), f32),
            vmem((events, 8, rows), f32),
            vmem((events, cb_count, 8, rows), f32),
            dma((STAGED,)),
            dma((STAGED,)),
            dma((STAGED,)),
            dma((RING,)),
            dma((RING,)),
            dma((RING, x_count)),
            dma((RING, x_count)),
            dma((RING, x_count)),
            dma((RING, x_count)),
            dma((RING,)),
            dma((RING,)),
            dma((parts, ra_count)),
            dma((parts, ra_count)),
            dma((parts, ra_count)),
            dma((parts, ra_count)),
            dma((events, cb_count)),
            dma((events, cb_count)),
        ],
        compiler_params=pltpu.CompilerParams(
            collective_id=0, has_side_effects=True, vmem_limit_bytes=62 * 1024 * 1024
        ),
        name="fused_sublayers",
    )(
        tokens.reshape(HALVES, rows, width),
        norm_gains,
        gate_weight,
        value_weight,
        gate_scale,
        value_scale,
        conv_gate,
        conv_value,
        down_weight,
        down_scale,
    )
    return result.reshape(HALVES * rows, width)


def solution(mesh):
    in_specs = (
        P("grp", "cb"),
        P(None, "cb"),
        P(None, "cb", "ra"),
        P(None, "cb", "ra"),
        P(None, "ra"),
        P(None, "ra"),
        P(None, None, "ra"),
        P(None, None, "ra"),
        P(None, "ra", "cb"),
        P(None, "cb"),
    )
    out_specs = P("grp", "cb")
    return jax.shard_map(
        functools.partial(on_device_any, mesh.shape["ra"], mesh.shape["cb"]), mesh=mesh, in_specs=in_specs, out_specs=out_specs, check_vma=False
    )
```

```python
import functools

import jax
import jax.numpy as jnp
from jax import lax
from jax.experimental import pallas as pl
from jax.experimental.pallas import tpu as pltpu
from jax.sharding import PartitionSpec as P

epsilon = 1e-06
residual_weight = 0.5


def causal_taps(projected, tap_weights):
    tap_count = tap_weights.shape[0]
    row_count = projected.shape[0]
    padded = jnp.pad(projected, ((tap_count - 1, 0), (0, 0)))
    result = jnp.zeros_like(projected)
    for tap_idx in range(tap_count):
        result = result + padded[tap_idx : tap_idx + row_count] * tap_weights[tap_idx]
    return result


def row_inverse(state_wide, model_width):
    squares = lax.psum(jnp.sum(state_wide * state_wide, axis=1, keepdims=True), "cb")
    return lax.rsqrt(squares / model_width + epsilon)


def on_device(
    tokens,
    norm_gains,
    gate_weight,
    value_weight,
    gate_scale,
    value_scale,
    conv_gate,
    conv_value,
    down_weight,
    down_scale,
):
    model_width = lax.axis_size("cb") * tokens.shape[1]
    layer_count = gate_weight.shape[0]
    current = tokens
    for layer_idx in range(layer_count):
        state_wide = current.astype(jnp.float32)
        inverse = row_inverse(state_wide, model_width)
        scaled = (state_wide * norm_gains[layer_idx]).astype(jnp.bfloat16)
        gate_part = jnp.dot(
            scaled, gate_weight[layer_idx].astype(jnp.bfloat16), preferred_element_type=jnp.float32
        )
        value_part = jnp.dot(
            scaled, value_weight[layer_idx].astype(jnp.bfloat16), preferred_element_type=jnp.float32
        )
        gate_sum, value_sum = (
            lax.psum_scatter(gate_part, "cb", scatter_dimension=1, tiled=True),
            lax.psum_scatter(value_part, "cb", scatter_dimension=1, tiled=True),
        )
        share_cols = gate_sum.shape[1]
        first_col = lax.axis_index("cb") * share_cols
        gate_cols = lax.dynamic_slice_in_dim(gate_scale[layer_idx], first_col, share_cols, 0)
        value_cols = lax.dynamic_slice_in_dim(value_scale[layer_idx], first_col, share_cols, 0)
        gate_taps = lax.dynamic_slice_in_dim(conv_gate[layer_idx], first_col, share_cols, 1)
        value_taps = lax.dynamic_slice_in_dim(conv_value[layer_idx], first_col, share_cols, 1)
        gate_pre = inverse * gate_cols * gate_sum
        value_pre = inverse * value_cols * value_sum
        hidden = (
            jax.nn.gelu(causal_taps(gate_pre, gate_taps), approximate=True)
            * causal_taps(value_pre, value_taps)
        ).astype(jnp.bfloat16)
        hidden = lax.all_gather(hidden, "cb", axis=1, tiled=True)
        partial_value = jnp.dot(
            hidden, down_weight[layer_idx].astype(jnp.bfloat16), preferred_element_type=jnp.float32
        )
        down_total = lax.psum(partial_value, "ra")
        current = (residual_weight * state_wide + down_scale[layer_idx] * down_total).astype(
            jnp.bfloat16
        )
    state_wide = current.astype(jnp.float32)
    inverse = row_inverse(state_wide, model_width)
    return (state_wide * inverse * norm_gains[layer_count]).astype(jnp.bfloat16)


HALVES = 2
CORES = 2
LANES = 128
CHUNK = 256
RING = 12
STAGED = 5
BUBBLES = 12
PAIR_SUM, GATED, PAIR_GATHER, DOWN = 2, 5, 8, 10
Z_SUM, Z_GATHER, Z_SCALE = 8, 13, 14


def fused_kernel(
    ra_count,
    cb_count,
    tokens,
    gains,
    gate_hbm,
    value_hbm,
    gate_scale,
    value_scale,
    conv_gate,
    conv_value,
    down_hbm,
    down_scale,
    out,
    gate_stage,
    value_stage,
    down_stage,
    wide_weight,
    down_weight,
    current,
    scaled,
    inverse,
    padded,
    carry,
    pair_send,
    pair_recv,
    pair_own,
    x_send,
    x_recv,
    hidden,
    acc,
    z_send,
    z_recv,
    z_own,
    sq_send,
    sq_recv,
    gate_sem,
    value_sem,
    down_sem,
    pair_ss,
    pair_rs,
    x_ss,
    x_rs,
    hx_ss,
    hx_rs,
    hp_ss,
    hp_rs,
    z_ss,
    z_rs,
    c_ss,
    c_rs,
    sq_ss,
    sq_rs,
):
    f32, bf16 = jnp.float32, jnp.bfloat16
    layers = gate_hbm.shape[0]
    chunks = gate_hbm.shape[2] // CHUNK
    taps = conv_gate.shape[1]
    rows = tokens.shape[1]
    width = tokens.shape[2]
    model_width = width * cb_count
    x_count = cb_count // CORES
    block = rows // cb_count
    z_block = rows // ra_count
    period = HALVES * chunks + BUBBLES
    last_item = layers * period - BUBBLES
    streamed = layers * chunks

    me_cb = lax.axis_index("cb")
    me_ra = lax.axis_index("ra")
    me_x, me_core = lax.div(me_cb, CORES), lax.rem(me_cb, CORES)
    partner = me_x * CORES + (1 - me_core)

    def others(count, me):
        return [lax.rem(me + step, count) for step in range(1, count)]

    def remote(src, dst, send, recv, axis, index):
        return pltpu.make_async_remote_copy(
            src_ref=src,
            dst_ref=dst,
            send_sem=send,
            recv_sem=recv,
            device_id={axis: index},
            device_id_type=pl.DeviceIdType.MESH,
        )

    def cb_of(x_index):
        return x_index * CORES + me_core

    def wide_copies(n):
        layer, chunk, slot = lax.div(n, chunks), lax.rem(n, chunks), lax.rem(n, STAGED)
        cols = pl.ds(pl.multiple_of(chunk * CHUNK, CHUNK), CHUNK)
        return (
            pltpu.make_async_copy(gate_hbm.at[layer, :, cols], gate_stage.at[slot], gate_sem.at[slot]),
            pltpu.make_async_copy(value_hbm.at[layer, :, cols], value_stage.at[slot], value_sem.at[slot]),
        )

    def down_copy(n):
        layer, chunk, slot = lax.div(n, chunks), lax.rem(n, chunks), lax.rem(n, STAGED)
        cols = pl.ds(pl.multiple_of(chunk * CHUNK, CHUNK), CHUNK)
        return pltpu.make_async_copy(down_hbm.at[layer, cols, :], down_stage.at[slot], down_sem.at[slot])

    for n in range(min(STAGED, streamed)):
        for copy in wide_copies(n):
            copy.start()
        down_copy(n).start()

    barrier = pltpu.get_barrier_semaphore()
    for axis, count, me in (("cb", cb_count, me_cb), ("ra", ra_count, me_ra)):
        for peer in others(count, me):
            pl.semaphore_signal(
                barrier, inc=1, device_id={axis: peer}, device_id_type=pl.DeviceIdType.MESH
            )
    pl.semaphore_wait(barrier, cb_count + ra_count - 2)

    def pair_copy(slot):
        return remote(
            pair_send.at[slot], pair_recv.at[slot], pair_ss.at[slot], pair_rs.at[slot], "cb", partner
        )

    def x_copy(slot, peer, source):
        return remote(
            x_send.at[slot, peer],
            x_recv.at[slot, source],
            x_ss.at[slot, peer],
            x_rs.at[slot, source],
            "cb",
            cb_of(peer),
        )

    def hx_copy(slot, peer, source):
        place = hidden.at[slot, me_core * x_count + source]
        return remote(place, place, hx_ss.at[slot, peer], hx_rs.at[slot, source], "cb", cb_of(peer))

    def hp_copy(slot, core):
        place = hidden.at[slot, pl.ds(core * x_count, x_count)]
        return remote(place, place, hp_ss.at[slot], hp_rs.at[slot], "cb", partner)

    def z_copy(part, peer, source):
        return remote(
            z_send.at[part, peer],
            z_recv.at[part, source],
            z_ss.at[part, peer],
            z_rs.at[part, source],
            "ra",
            peer,
        )

    def c_copy(part, layer, half, peer, source):
        place = current.at[layer, half, source]
        return remote(place, place, c_ss.at[part, peer], c_rs.at[part, source], "ra", peer)

    def sq_copy(event, peer, source):
        return remote(
            sq_send.at[event], sq_recv.at[event, source], sq_ss.at[event, peer], sq_rs.at[event, source], "cb", peer
        )

    def scale_rows(layer, half):
        event = layer * HALVES + half
        wide = current[layer, half].reshape(rows, width).astype(f32)
        scaled[half] = (wide * gains[pl.ds(layer, 1), :]).astype(bf16)
        squares = jnp.sum(wide * wide, axis=1, keepdims=True)
        sq_send[event] = jnp.broadcast_to(squares, (rows, LANES)).T[:8]
        for peer in others(cb_count, me_cb):
            sq_copy(event, peer, me_cb).start()

    def finish_squares(layer, half):
        event = layer * HALVES + half
        total = sq_send[event]
        for peer in others(cb_count, me_cb):
            copy = sq_copy(event, peer, peer)
            copy.wait_send()
            copy.wait_recv()
            total = total + sq_recv[event, peer]
        row = lax.rsqrt(total / model_width + epsilon)
        inverse[half] = jnp.broadcast_to(row[:1], (LANES, rows)).T

    for half in range(HALVES):
        current[0, half] = tokens[half].reshape(ra_count, z_block, width)
        scale_rows(0, half)
    for half in range(HALVES):
        finish_squares(0, half)

    def place_of(item):
        layer, rest = lax.div(item, period), lax.rem(item, period)
        half, chunk = lax.div(rest, chunks), lax.rem(rest, chunks)
        ordinal = layer * (HALVES * chunks) + rest
        return layer, half, chunk, lax.rem(ordinal, RING)

    def project(layer, half, chunk, slot):
        n = layer * chunks + chunk

        @pl.when(half == 0)
        def _():
            stage = lax.rem(n, STAGED)
            for copy in wide_copies(n):
                copy.wait()
            wide_weight[chunk, :, :CHUNK] = gate_stage[stage].astype(bf16)
            wide_weight[chunk, :, CHUNK:] = value_stage[stage].astype(bf16)

            @pl.when(n + STAGED < streamed)
            def _():
                for copy in wide_copies(n + STAGED):
                    copy.start()

        product = jnp.dot(scaled[half], wide_weight[chunk], preferred_element_type=f32)
        inv = inverse[half]
        cols = pl.ds(pl.multiple_of(chunk * CHUNK, CHUNK), CHUNK)
        one = pl.ds(layer, 1)
        scales = jnp.concatenate([gate_scale[one, cols], value_scale[one, cols]], axis=1)
        weights = jnp.concatenate([conv_gate[layer, :, cols], conv_value[layer, :, cols]], axis=1)
        wide_inv = jnp.concatenate([inv] * (2 * CHUNK // LANES), axis=1)
        pre = product * wide_inv * scales
        before = carry[chunk]
        padded[:8] = jnp.where(half == 0, jnp.zeros_like(before), before)
        padded[8:] = pre
        carry[chunk] = pre[rows - 8 :]
        total = jnp.zeros_like(pre)
        for tap in range(taps):
            total = total + padded[pl.ds(8 - (taps - 1) + tap, rows), :] * weights[tap : tap + 1]
        part = rows // CORES
        for core in range(CORES):
            piece = total[core * part : (core + 1) * part]

            @pl.when(me_core == core)
            def _():
                pair_own[slot] = piece.reshape(x_count, block, 2 * CHUNK)

            @pl.when(me_core != core)
            def _():
                pair_send[slot] = piece.astype(bf16).reshape(x_count, block, 2 * CHUNK)

        pair_copy(slot).start()

    def pair_sum(layer, half, chunk, slot):
        pair_copy(slot).wait()
        both = pair_own[slot] + pair_recv[slot].astype(f32)
        pair_own[slot] = both
        x_send[slot] = both.astype(bf16)
        for peer in others(x_count, me_x):
            x_copy(slot, peer, me_x).start()

    def gated(layer, half, chunk, slot):
        total = pair_own[slot, me_x]
        for peer in others(x_count, me_x):
            copy = x_copy(slot, peer, peer)
            copy.wait_send()
            copy.wait_recv()
            total = total + x_recv[slot, peer].astype(f32)
        unit = jax.nn.gelu(total[:, :CHUNK], approximate=True) * total[:, CHUNK:]
        hidden[slot, me_core * x_count + me_x] = unit.astype(bf16)
        for peer in others(x_count, me_x):
            hx_copy(slot, peer, me_x).start()

    def pair_gather(layer, half, chunk, slot):
        for peer in others(x_count, me_x):
            hx_copy(slot, peer, me_x).wait_send()
            hx_copy(slot, peer, peer).wait_recv()
        hp_copy(slot, me_core).start()

    def project_down(layer, half, chunk, slot):
        n = layer * chunks + chunk

        @pl.when(half == 0)
        def _():
            stage = lax.rem(n, STAGED)
            down_copy(n).wait()
            down_weight[chunk] = down_stage[stage].astype(bf16)

            @pl.when(n + STAGED < streamed)
            def _():
                down_copy(n + STAGED).start()

        hp_copy(slot, me_core).wait_send()
        hp_copy(slot, 1 - me_core).wait_recv()
        product = jnp.dot(
            hidden[slot].reshape(rows, CHUNK), down_weight[chunk], preferred_element_type=f32
        ).reshape(ra_count, z_block, width)

        @pl.when(chunk == 0)
        def _():
            acc[...] = product

        @pl.when(chunk > 0)
        def _():
            acc[...] += product

        @pl.when(chunk == chunks - 1)
        def _():
            part = layer * HALVES + half
            z_send[part] = acc[...].astype(bf16)
            z_own[part] = acc[me_ra]
            for peer in others(ra_count, me_ra):
                z_copy(part, peer, me_ra).start()

    def z_sum(layer, half, chunk, slot):
        part = layer * HALVES + half
        total = z_own[part]
        for peer in others(ra_count, me_ra):
            copy = z_copy(part, peer, peer)
            copy.wait_send()
            copy.wait_recv()
            total = total + z_recv[part, peer].astype(f32)
        kept = residual_weight * current[layer, half, me_ra].astype(f32)
        current[layer + 1, half, me_ra] = (kept + down_scale[pl.ds(layer, 1), :] * total).astype(bf16)
        for peer in others(ra_count, me_ra):
            c_copy(part, layer + 1, half, peer, me_ra).start()

    def z_gather(layer, half, chunk, slot):
        part = layer * HALVES + half
        for peer in others(ra_count, me_ra):
            c_copy(part, layer + 1, half, peer, me_ra).wait_send()
            c_copy(part, layer + 1, half, peer, peer).wait_recv()
        scale_rows(layer + 1, half)

    def z_scale(layer, half, chunk, slot):
        finish_squares(layer + 1, half)

        @pl.when(layer == layers - 1)
        def _():
            wide = current[layers, half].reshape(rows, width).astype(f32)
            inv = jnp.concatenate([inverse[half]] * (width // LANES), axis=1)
            out[half] = (wide * inv * gains[pl.ds(layers, 1), :]).astype(bf16)

    stages = (
        (DOWN + Z_SCALE, True, z_scale),
        (DOWN + Z_GATHER, True, z_gather),
        (DOWN + Z_SUM, True, z_sum),
        (PAIR_GATHER, False, pair_gather),
        (GATED, False, gated),
        (PAIR_SUM, False, pair_sum),
        (0, False, project),
        (DOWN, False, project_down),
    )
    assert DOWN + Z_SCALE <= chunks + BUBBLES + 1

    def step(index, _):
        for delay, at_end, stage in stages:
            item = index - delay
            rest = lax.rem(item + period, period)
            valid = (item >= 0) & (item < last_item) & (rest < HALVES * chunks)
            if at_end:
                valid = valid & (lax.rem(rest, chunks) == chunks - 1)

            @pl.when(valid)
            def _(stage=stage, item=item):
                stage(*place_of(item))

        return 0

    lax.fori_loop(0, last_item + DOWN + Z_SCALE, step, 0)


def fits(ra_count, cb_count, tokens, gate_weight, conv_gate):
    rows = tokens.shape[0] // HALVES
    return (
        cb_count % CORES == 0
        and cb_count > CORES
        and ra_count > 1
        and tokens.shape[0] % HALVES == 0
        and rows % LANES == 0
        and (rows // LANES) == 1
        and rows % (16 * cb_count) == 0
        and rows % (16 * ra_count) == 0
        and tokens.shape[1] % LANES == 0
        and gate_weight.shape[2] % CHUNK == 0
        and gate_weight.shape[2] // CHUNK + BUBBLES + 1 >= DOWN + Z_SCALE
        and conv_gate.shape[1] <= 9
    )


def on_device_any(ra_count, cb_count, *args):
    (
        tokens,
        norm_gains,
        gate_weight,
        value_weight,
        gate_scale,
        value_scale,
        conv_gate,
        conv_value,
        down_weight,
        down_scale,
    ) = args
    if not fits(ra_count, cb_count, tokens, gate_weight, conv_gate):
        return on_device(*args)
    f32, bf16 = jnp.float32, jnp.bfloat16
    layers, width, units = gate_weight.shape
    rows = tokens.shape[0] // HALVES
    chunks = units // CHUNK
    x_count = cb_count // CORES
    block, z_block = rows // cb_count, rows // ra_count
    parts, events = layers * HALVES, (layers + 1) * HALVES
    vmem, dma = pltpu.VMEM, pltpu.SemaphoreType.DMA
    in_vmem, in_hbm = pl.BlockSpec(memory_space=pltpu.VMEM), pl.BlockSpec(memory_space=pl.ANY)
    result = pl.pallas_call(
        functools.partial(fused_kernel, ra_count, cb_count),
        out_shape=jax.ShapeDtypeStruct((HALVES, rows, width), bf16),
        in_specs=[in_vmem, in_vmem, in_hbm, in_hbm] + [in_vmem] * 4 + [in_hbm, in_vmem],
        out_specs=in_vmem,
        scratch_shapes=[
            vmem((STAGED, width, CHUNK), f32),
            vmem((STAGED, width, CHUNK), f32),
            vmem((STAGED, CHUNK, width), f32),
            vmem((chunks, width, 2 * CHUNK), bf16),
            vmem((chunks, CHUNK, width), bf16),
            vmem((layers + 1, HALVES, ra_count, z_block, width), bf16),
            vmem((HALVES, rows, width), bf16),
            vmem((HALVES, rows, LANES), f32),
            vmem((rows + 8, 2 * CHUNK), f32),
            vmem((chunks, 8, 2 * CHUNK), f32),
            vmem((RING, x_count, block, 2 * CHUNK), bf16),
            vmem((RING, x_count, block, 2 * CHUNK), bf16),
            vmem((RING, x_count, block, 2 * CHUNK), f32),
            vmem((RING, x_count, block, 2 * CHUNK), bf16),
            vmem((RING, x_count, block, 2 * CHUNK), bf16),
            vmem((RING, cb_count, block, CHUNK), bf16),
            vmem((ra_count, z_block, width), f32),
            vmem((parts, ra_count, z_block, width), bf16),
            vmem((parts, ra_count, z_block, width), bf16),
            vmem((parts, z_block, width), f32),
            vmem((events, 8, rows), f32),
            vmem((events, cb_count, 8, rows), f32),
            dma((STAGED,)),
            dma((STAGED,)),
            dma((STAGED,)),
            dma((RING,)),
            dma((RING,)),
            dma((RING, x_count)),
            dma((RING, x_count)),
            dma((RING, x_count)),
            dma((RING, x_count)),
            dma((RING,)),
            dma((RING,)),
            dma((parts, ra_count)),
            dma((parts, ra_count)),
            dma((parts, ra_count)),
            dma((parts, ra_count)),
            dma((events, cb_count)),
            dma((events, cb_count)),
        ],
        compiler_params=pltpu.CompilerParams(
            collective_id=0, has_side_effects=True, vmem_limit_bytes=62 * 1024 * 1024
        ),
        name="fused_sublayers",
    )(
        tokens.reshape(HALVES, rows, width),
        norm_gains,
        gate_weight,
        value_weight,
        gate_scale,
        value_scale,
        conv_gate,
        conv_value,
        down_weight,
        down_scale,
    )
    return result.reshape(HALVES * rows, width)


def solution(mesh):
    in_specs = (
        P("grp", "cb"),
        P(None, "cb"),
        P(None, "cb", "ra"),
        P(None, "cb", "ra"),
        P(None, "ra"),
        P(None, "ra"),
        P(None, None, "ra"),
        P(None, None, "ra"),
        P(None, "ra", "cb"),
        P(None, "cb"),
    )
    out_specs = P("grp", "cb")
    return jax.shard_map(
        functools.partial(on_device_any, mesh.shape["ra"], mesh.shape["cb"]), mesh=mesh, in_specs=in_specs, out_specs=out_specs, check_vma=False
    )
```
